32 devices in a mesh: grp: 2 (over y), sp: 4 (over z), tp: 4 (over x, core).
Axes of the slice: x: 2, y: 2, z: 4, core: 2. Of those that a mesh axis runs over, the one named last changes fastest.
Arguments:
- tokens: bfloat16 [6144, 2048], P(('grp', 'sp'), 'tp'), parts along dimension 0, may hold values from -8 to 8
- norm_gain: float32 [2, 2048], replicated, may hold values from 0.1 to 1.9
- w_value: bfloat16 [2, 2048, 2048], P(None, 'sp', 'tp'), may hold values from -0.125 to 0.125
- w_gate: bfloat16 [2, 2048, 2048], P(None, 'sp', 'tp'), may hold values from -0.125 to 0.125
- taps: float32 [2, 31, 2048], P(None, None, 'tp'), may hold values from -2 to 2
- ln_gain: float32 [2, 2048], P(None, 'tp'), may hold values from 0.1 to 1.9
- ln_shift: float32 [2, 2048], P(None, 'tp'), may hold values from -3 to 3
- w_out: bfloat16 [2, 2048, 2048], P(None, 'sp', 'tp'), may hold values from -0.125 to 0.125
Outputs:
- stream_out: bfloat16 [6144, 2048], P(('grp', 'sp'), 'tp'), parts along dimension 0
The draws below stay inside these ranges and needn't reach their ends.
There are 2 independent parts, one for each index of `grp`. The reference program is written for one: setup_inputs(seed, part) draws one part's arguments, and reference() takes and returns one part's arrays. A program takes and returns all parts, laid end to end along the dimension named above; an argument that names none is the same for every part. Nothing has to cross between parts.
All inputs are finite; a program needn't handle non-finite values.
Results may differ from the reference program's by a relative error of at most 0.012.
Values may be sent and summed in bfloat16 or wider, within the bound.
No kernel may reach another device: no remote copies, remote signals or barrier semaphores. Data moves between devices by JAX's collectives and lax.ppermute only.
A program may use at most 64 MiB of HBM per device.

```python
import jax
import jax.numpy as jnp
from jax import lax

D = 2048
C = 2048
KERNEL = 31
LAYERS = 2
TOKENS = 3072


def draw_tokens(key, part):
    first, second = jax.random.split(jax.random.fold_in(key, 11), 2)
    ramp = jnp.exp(jnp.linspace(-0.7, 0.7, D))
    rough = jnp.exp(jax.random.uniform(second, (D,), minval=-0.5, maxval=0.5))
    base = jnp.clip(jax.random.normal(first, (TOKENS, D)), -2.4, 2.4)
    return (base * ramp * rough).astype(jnp.bfloat16)


def draw_taps(key, part):
    first, second = jax.random.split(jax.random.fold_in(key, 23), 2)
    ramp = jnp.exp(jnp.linspace(-0.7, 0.7, C))
    rough = jnp.exp(jax.random.uniform(second, (C,), minval=-0.4, maxval=0.4))
    base = jnp.clip(jax.random.normal(first, (LAYERS, KERNEL, C)), -3.0, 3.0)
    return (base * KERNEL ** (-0.5) * ramp * rough).astype(jnp.float32)


def block_scale(stream_key, dims, cuts, smallest, top_value):
    def one(dim, blocks):
        draws = jax.random.uniform(jax.random.fold_in(jax.random.fold_in(stream_key, 6), dim), (blocks,), jnp.float32, smallest / len(cuts), top_value / len(cuts))
        return jnp.repeat(jnp.exp(draws), dims[dim] // blocks).reshape((-1,) + (1,) * (len(dims) - dim - 1))

    factor_of = one(*cuts[0])
    for cut in cuts[1:]:
        factor_of = factor_of * one(*cut)
    return factor_of


def normal_values(stream_key, shape, deviation, most, shards=(), dtype=jnp.bfloat16):
    array = deviation * jax.random.normal(stream_key, shape, jnp.float32)
    if shards:
        array = array * block_scale(stream_key, shape, shards, -0.22, 0.18)
    return jnp.clip(array, -most, most).astype(dtype)


def setup_inputs(seed: int = 0, part: int = 0) -> dict:
    keys = jax.random.split(jax.random.key(seed), 9)
    part_keys = jax.random.split(jax.random.fold_in(keys[8], part), 9)
    tokens = draw_tokens(jax.random.fold_in(jax.random.fold_in(keys[8], part), 71), part)
    norm_gain = jnp.clip(1.0 + 0.18 * jax.random.normal(keys[1], (LAYERS, D), jnp.float32), 0.1, 1.9)
    w_value = normal_values(keys[2], (LAYERS, D, C), D ** -0.5, 0.125, ((1, 4), (2, 4)))
    w_gate = normal_values(keys[3], (LAYERS, D, C), D ** -0.5, 0.125, ((1, 4), (2, 4)))
    taps = draw_taps(jax.random.fold_in(keys[8], 71), part)
    ln_gain = jnp.clip(1.0 + 0.18 * jax.random.normal(keys[5], (LAYERS, C), jnp.float32), 0.1, 1.9)
    ln_shift = normal_values(keys[6], (LAYERS, C), 0.5, 3.0, ((1, 4),), jnp.float32)
    w_out = normal_values(keys[7], (LAYERS, C, D), C ** -0.5, 0.125, ((1, 4), (2, 4)))
    return {"tokens": tokens, "norm_gain": norm_gain, "w_value": w_value, "w_gate": w_gate, "taps": taps, "ln_gain": ln_gain, "ln_shift": ln_shift, "w_out": w_out}


def reference(tokens, norm_gain, w_value, w_gate, taps, ln_gain, ln_shift, w_out):
    half = (KERNEL - 1) // 2
    stream = tokens
    for layer in range(LAYERS):
        wide = stream.astype(jnp.float32)
        meansq = lax.optimization_barrier(jnp.mean(wide * wide, axis=1, keepdims=True))
        normed = (wide * lax.rsqrt(meansq + 1e-06) * norm_gain[layer]).astype(jnp.bfloat16)
        value = jnp.dot(normed, w_value[layer], preferred_element_type=jnp.float32)
        gate = jnp.dot(normed, w_gate[layer], preferred_element_type=jnp.float32)
        glu = (value * jax.nn.sigmoid(gate)).astype(jnp.bfloat16)
        padded = jnp.pad(glu.astype(jnp.float32), ((half, half), (0, 0)))
        count = glu.shape[0]
        conv = jnp.zeros(glu.shape, jnp.float32)
        for step in range(KERNEL):
            conv = conv + taps[layer, step][None, :] * padded[step:step + count]
        mean_c = lax.optimization_barrier(jnp.mean(conv, axis=1, keepdims=True))
        var_c = lax.optimization_barrier(jnp.mean(conv * conv, axis=1, keepdims=True)) - mean_c * mean_c
        shaped = (conv - mean_c) * lax.rsqrt(var_c + 1e-05) * ln_gain[layer] + ln_shift[layer]
        act = jax.nn.silu(shaped).astype(jnp.bfloat16)
        update = jnp.dot(act, w_out[layer], preferred_element_type=jnp.float32)
        stream = (stream.astype(jnp.float32) + update).astype(jnp.bfloat16)
    return stream
```

```python
import functools

import jax
import jax.numpy as jnp
from jax import lax
from jax.experimental import pallas as pl
from jax.experimental.pallas import tpu as pltpu
from jax.sharding import PartitionSpec as P

CORES = 2
LANES = 128
BF16 = jnp.bfloat16
F32 = jnp.float32


def ring(x, axis, step):
    n = lax.axis_size(axis)
    return lax.ppermute(x, axis, [(i, (i + step) % n) for i in range(n)])


def line(x, axis, step):
    n = lax.axis_size(axis)
    return lax.ppermute(x, axis, [(i, i + step) for i in range(n) if 0 <= i + step < n])


def sibling(x):
    n = lax.axis_size("tp")
    return lax.ppermute(x, "tp", [(i, i ^ 1) for i in range(n)])


def chip_shift(x, step):
    n = lax.axis_size("tp")
    pairs = [(i, (i + CORES * step) % n) for i in range(n)]
    return lax.ppermute(x, "tp", pairs)


def feature_slot(shift, core):
    n = lax.axis_size("tp")
    me = lax.axis_index("tp")
    chip, mine = lax.div(me, CORES), lax.rem(me, CORES)
    chip = lax.rem(chip - shift + n // CORES, n // CORES)
    return chip * CORES + (mine if core == 0 else 1 - mine)


def source_row(shift):
    n = lax.axis_size("sp")
    return lax.rem(lax.axis_index("sp") - shift + n, n)


def params(limit=48):
    return pltpu.CompilerParams(vmem_limit_bytes=limit * 2**20)


def vmem(count):
    return [pl.BlockSpec(memory_space=pltpu.VMEM)] * count


def norm_kernel(shifts, width, gain_ref, *refs):
    blocks, out_ref = refs[:-1], refs[-1]
    rows = out_ref.shape[0]
    total = out_ref.shape[1]
    tile = 16
    slots = [feature_slot(e, c) for e in range(shifts) for c in range(CORES)]

    def body(i, carry):
        at = pl.ds(pl.multiple_of(i * tile, tile), tile)
        parts = [b[at, :].astype(F32) for b in blocks]
        square = sum(p * p for p in parts)
        scale = lax.rsqrt(jnp.sum(square, axis=1, keepdims=True) / total + 1e-06)
        for slot, part in zip(slots, parts):
            cols = pl.ds(pl.multiple_of(slot * width, LANES), width)
            out_ref[at, cols] = (part * scale * gain_ref[:, cols]).astype(BF16)
        return carry

    lax.fori_loop(0, rows // tile, body, 0, unroll=2)


def normalize(blocks, gain):
    shifts = len(blocks)
    flat = [b for pair in blocks for b in pair]
    rows, width = flat[0].shape
    total = width * len(flat)
    return pl.pallas_call(
        functools.partial(norm_kernel, shifts, width),
        out_shape=jax.ShapeDtypeStruct((rows, total), BF16),
        in_specs=vmem(1 + len(flat)),
        out_specs=vmem(1)[0],
        compiler_params=params(),
        cost_estimate=pl.CostEstimate(
            flops=rows * total * 400, bytes_accessed=4 * rows * total, transcendentals=0
        ),
        name="norm",
    )(gain, *flat)


def conv_strip(glu_ref, taps, out_ref, cols, offset):
    kernel = taps.shape[0]
    rows = out_ref.shape[0]
    spread = [jnp.broadcast_to(taps[k : k + 1, :], (8, LANES)) for k in range(kernel)]
    by_shift = [
        [((k + offset) // 8, k) for k in range(kernel) if (k + offset) % 8 == s] for s in range(8)
    ]
    reach = (kernel - 1 + offset) // 8 + 1
    row_id = lax.broadcasted_iota(jnp.int32, (8, LANES), 0)

    def partials(i):
        window = [
            glu_ref[pl.ds(pl.multiple_of((i + q) * 8, 8), 8), cols] for q in range(reach)
        ]
        out = []
        for s, members in enumerate(by_shift):
            acc = None
            for q, k in members:
                term = spread[k] * window[q]
                acc = term if acc is None else acc + term
            if acc is None:
                acc = jnp.zeros((8, LANES), F32)
            out.append(acc if s == 0 else pltpu.roll(acc, 8 - s, 0))
        return out

    def merge(now, later):
        acc = now[0]
        for s in range(1, 8):
            acc = acc + jnp.where(row_id < 8 - s, now[s], later[s])
        return acc

    def body(j, now):
        middle = partials(2 * j + 1)
        later = partials(2 * j + 2)
        pair = jnp.concatenate([merge(now, middle), merge(middle, later)], axis=0)
        out_ref[pl.ds(pl.multiple_of(j * 16, 16), 16), cols] = pair.astype(BF16)
        return later

    lax.fori_loop(0, rows // 16, body, partials(0))


def glu_conv_kernel(spans, pad, x_ref, *refs):
    taps = refs[:CORES]
    weights = refs[CORES:-2]
    out_ref, glu_ref = refs[-2:]
    groups = len(weights) // (CORES * spans)
    depth, width = weights[0].shape
    kernel = taps[0].shape[0]
    offset = pad - (kernel - 1) // 2
    first = (lax.axis_index("grp") == 0) | (lax.axis_size("grp") != 2)
    at = [pl.ds(pl.multiple_of(source_row(d) * depth, LANES), depth) for d in range(spans)]
    for core in range(CORES):
        prods = []
        for side in range(groups):
            acc = None
            for d in range(spans):
                w = weights[(core * groups + side) * spans + d]
                term = jnp.dot(x_ref[:, at[d]], w[...], preferred_element_type=F32)
                acc = term if acc is None else acc + term
            prods.append(acc)
        value = jnp.where(first, prods[0], prods[1])
        gate = jnp.where(first, prods[1], prods[0])
        glu_ref[:, core * width : (core + 1) * width] = value * jax.nn.sigmoid(gate)
        for strip in range(width // LANES):
            conv_strip(
                glu_ref,
                taps[core][:, strip * LANES : (strip + 1) * LANES],
                out_ref,
                slice(core * width + strip * LANES, core * width + (strip + 1) * LANES),
                offset,
            )


def glu_conv(x, taps, weights, pad):
    spans = len(weights[0][0])
    flat = [w for core in weights for side in core for w in side]
    rows = x.shape[0]
    width = flat[0].shape[1]
    flops = 2 * rows * x.shape[1] * width * CORES * 2
    return pl.pallas_call(
        functools.partial(glu_conv_kernel, spans, pad),
        out_shape=jax.ShapeDtypeStruct((rows - 2 * pad, CORES * width), BF16),
        in_specs=vmem(1 + CORES + len(flat)),
        out_specs=vmem(1)[0],
        scratch_shapes=[pltpu.VMEM((rows, CORES * width), F32)],
        compiler_params=params(),
        cost_estimate=pl.CostEstimate(
            flops=flops, bytes_accessed=2 * rows * x.shape[1], transcendentals=0
        ),
        name="glu_conv",
    )(x, *taps, *flat)


def act_kernel(shifts, halves, *refs):
    lns = refs[:shifts]
    blocks = refs[shifts:-1]
    out_ref = refs[-1]
    rows, total = out_ref.shape
    width = blocks[0].shape[1] // CORES
    tile = 16

    def body(i, carry):
        at = pl.ds(pl.multiple_of(i * tile, tile), tile)
        parts = [b[at, :].astype(F32) for b in blocks]
        mean = jnp.sum(sum(parts), axis=1, keepdims=True) / total
        square = jnp.sum(sum(p * p for p in parts), axis=1, keepdims=True) / total
        scale = lax.rsqrt(square - mean * mean + 1e-05)
        for e in range(shifts):
            for h in range(halves):
                part = parts[e * halves + h]
                for core in range(CORES):
                    own = part[:, core * width : (core + 1) * width]
                    gain = lns[e][core : core + 1, h * width : (h + 1) * width]
                    bias = lns[e][CORES + core : CORES + core + 1, h * width : (h + 1) * width]
                    shaped = (own - mean) * scale * gain + bias
                    start = feature_slot(e, core) * (width * halves) + h * width
                    cols = pl.ds(pl.multiple_of(start, LANES), width)
                    out_ref[at, cols] = (shaped * jax.nn.sigmoid(shaped)).astype(BF16)
        return carry

    lax.fori_loop(0, rows // tile, body, 0, unroll=2)


def activation(lns, blocks):
    shifts, halves = len(blocks), len(blocks[0])
    flat = [b for pair in blocks for b in pair]
    rows = flat[0].shape[0]
    total = sum(b.shape[1] for b in flat)
    return pl.pallas_call(
        functools.partial(act_kernel, shifts, halves),
        out_shape=jax.ShapeDtypeStruct((rows, total), BF16),
        in_specs=vmem(len(lns) + len(flat)),
        out_specs=vmem(1)[0],
        compiler_params=params(),
        cost_estimate=pl.CostEstimate(
            flops=rows * total * 800, bytes_accessed=4 * rows * total, transcendentals=0
        ),
        name="act",
    )(*lns, *flat)


def out_kernel(spans, pad, mask, span_rows, act_ref, res_ref, *refs):
    weights, out_ref = refs[:-1], refs[-1]
    sides = len(weights) // spans
    rows = out_ref.shape[0]
    depth = weights[0].shape[0]
    group = lax.axis_index("grp")
    acc = res_ref[pad : pad + rows, :].astype(F32)
    for d in range(spans):
        for side in range(sides):
            start = source_row(d) * (depth * sides)
            if sides > 1:
                start = start + (group if side == 0 else 1 - group) * depth
            at = pl.ds(pl.multiple_of(start, LANES), depth)
            w = weights[side * spans + d]
            acc = acc + jnp.dot(act_ref[:, at], w[...], preferred_element_type=F32)
    if mask:
        block = lax.axis_index("sp") * CORES + lax.rem(lax.axis_index("tp"), CORES)
        row = lax.broadcasted_iota(jnp.int32, (rows, 1), 0) - mask + block * span_rows
        inside = (row >= 0) & (row < span_rows * CORES * lax.axis_size("sp"))
        acc = jnp.where(inside, acc, 0.0)
    out_ref[...] = acc.astype(BF16)


def project_out(act, res, weights, pad, mask, span_rows):
    spans = len(weights[0])
    flat = [w for side in weights for w in side]
    rows = act.shape[0]
    width = res.shape[1]
    return pl.pallas_call(
        functools.partial(out_kernel, spans, pad, mask, span_rows),
        out_shape=jax.ShapeDtypeStruct((rows, width), BF16),
        in_specs=vmem(2 + len(flat)),
        out_specs=vmem(1)[0],
        compiler_params=params(),
        cost_estimate=pl.CostEstimate(
            flops=2 * rows * act.shape[1] * width,
            bytes_accessed=2 * rows * act.shape[1],
            transcendentals=0,
        ),
        name="out",
    )(act, res, *flat)


class Mover:
    def __init__(self):
        self.last = None

    def gather(self, mine, other):
        n = lax.axis_size("sp")
        if self.last is not None:
            mine, _ = lax.optimization_barrier((mine, self.last))
        own = [None] * n
        own[0] = mine
        upward, downward = n // 2, n - 1 - n // 2
        held = mine
        for d in range(1, upward + 1):
            held = ring(held, "sp", 1)
            own[d] = held
            if d == 1:
                self.last = held
        held = mine
        for d in range(1, downward + 1):
            held = ring(held, "sp", -1)
            own[n - d] = held
        if other is None:
            sides = [own]
        else:
            sides = [own, [other] + [ring(w, "grp", 1) for w in own[1:]]]
        return sides


def shards(tokens, norm_gain, w_value, w_gate, taps, ln_gain, ln_shift, w_out):
    layers = w_value.shape[0]
    kernel = taps.shape[1]
    half = (kernel - 1) // 2
    pad = -(-half // 16) * 16
    count, width = tokens.shape
    rows = count // CORES
    edge = pad * layers
    chips = lax.axis_size("tp") // CORES
    sp = lax.axis_size("sp")
    core = lax.rem(lax.axis_index("tp"), CORES)
    group = lax.axis_index("grp")
    depth = w_value.shape[1]
    chan = w_value.shape[2]
    halves = 2 if chan % (2 * LANES) == 0 else 1
    wide = chan // halves
    paired = lax.axis_size("grp") == 2
    split_rows = paired and (depth // 2) % LANES == 0

    sib_value, sib_gate, sib_out = sibling(w_value), sibling(w_gate), sibling(w_out)
    vectors = jnp.concatenate([taps, ln_gain[:, None], ln_shift[:, None]], axis=1)
    sib_vectors = sibling(vectors)
    lns_own = jnp.concatenate(
        [
            vectors[:, kernel : kernel + 1],
            sib_vectors[:, kernel : kernel + 1],
            vectors[:, kernel + 1 :],
            sib_vectors[:, kernel + 1 :],
        ],
        axis=1,
    )
    lns = [lns_own] + [chip_shift(lns_own, e) for e in range(1, chips)]

    before = line(tokens[count - edge :], "sp", 1)
    after = line(tokens[:edge], "sp", -1)
    extended = jnp.concatenate([before, tokens, after], axis=0)
    span = rows + 2 * edge
    own = lax.dynamic_slice_in_dim(extended, core * rows, span, 0)
    theirs = lax.dynamic_slice_in_dim(extended, (1 - core) * rows, span, 0)
    stream = [own, sibling(theirs)]

    mover = Mover()
    gathered = []
    for layer in range(layers):
        pieces = []
        for h in range(halves):
            cols = slice(h * wide, (h + 1) * wide)
            v, g = w_value[layer][:, cols], w_gate[layer][:, cols]
            sv, sg = sib_value[layer][:, cols], sib_gate[layer][:, cols]
            if paired:
                first = group == 0
                mine, other = jnp.where(first, v, g), jnp.where(first, g, v)
                smine, sother = jnp.where(first, sv, sg), jnp.where(first, sg, sv)
                sides = mover.gather(mine, other)
                sib = [
                    [smine] + [sibling(w) for w in sides[0][1:]],
                    [sother] + [sibling(w) for w in sides[1][1:]],
                ]
            else:
                sides = [mover.gather(v, None)[0], mover.gather(g, None)[0]]
                sib = [
                    [sv] + [sibling(w) for w in sides[0][1:]],
                    [sg] + [sibling(w) for w in sides[1][1:]],
                ]
            pieces.append([sides, sib])
        if split_rows:
            cut = depth // 2
            take = lambda w, at: lax.dynamic_slice_in_dim(w, at * cut, cut, 0)
            sides = mover.gather(take(w_out[layer], group), take(w_out[layer], 1 - group))
            starts = [take(sib_out[layer], group), take(sib_out[layer], 1 - group)]
        else:
            sides = mover.gather(w_out[layer], None)
            starts = [sib_out[layer]]
        sib = [[s] + [sibling(w) for w in side[1:]] for s, side in zip(starts, sides)]
        gathered.append((pieces, [sides, sib]))

    for layer in range(layers):
        last = layer == layers - 1
        pieces, closing = gathered[layer]
        blocks = [stream] + [[chip_shift(s, e) for s in stream] for e in range(1, chips)]
        normed = normalize(blocks, norm_gain[layer][None, :])
        convs = []
        for h in range(halves):
            cols = slice(h * wide, (h + 1) * wide)
            layer_taps = [vectors[layer, :kernel, cols], sib_vectors[layer, :kernel, cols]]
            convs.append(glu_conv(normed, layer_taps, pieces[h], pad))
        moved = [convs] + [[chip_shift(c, e) for c in convs] for e in range(1, chips)]
        act = activation([v[layer] for v in lns], moved)
        mask = 0 if last else pad * (layers - 1 - layer)
        order = (1, 0) if last else (0, 1)
        new = [None, None]
        for c in order:
            new[c] = project_out(act, stream[c], closing[c], pad, mask, rows)
        stream = new

    arrived = sibling(stream[1])
    return jnp.where(
        core == 0,
        jnp.concatenate([stream[0], arrived], axis=0),
        jnp.concatenate([arrived, stream[0]], axis=0),
    )


def solution(mesh):
    return jax.shard_map(
        shards,
        mesh=mesh,
        in_specs=(
            P(("grp", "sp"), "tp"),
            P(),
            P(None, "sp", "tp"),
            P(None, "sp", "tp"),
            P(None, None, "tp"),
            P(None, "tp"),
            P(None, "tp"),
            P(None, "sp", "tp"),
        ),
        out_specs=P(("grp", "sp"), "tp"),
        check_vma=False,
    )
```

```python
import functools

import jax
import jax.numpy as jnp
from jax import lax
from jax.experimental import pallas as pl
from jax.experimental.pallas import tpu as pltpu
from jax.sharding import PartitionSpec as P


CORES = 2
LANES = 128
BF16 = jnp.bfloat16
F32 = jnp.float32


def ring(x, axis, step):
    n = lax.axis_size(axis)
    return lax.ppermute(x, axis, [(i, (i + step) % n) for i in range(n)])


def line(x, axis, step):
    n = lax.axis_size(axis)
    return lax.ppermute(x, axis, [(i, i + step) for i in range(n) if 0 <= i + step < n])


def sibling(x):
    n = lax.axis_size("tp")
    return lax.ppermute(x, "tp", [(i, i ^ 1) for i in range(n)])


def chip_shift(x, step):
    n = lax.axis_size("tp")
    pairs = [(i, (i + CORES * step) % n) for i in range(n)]
    return lax.ppermute(x, "tp", pairs)


def feature_slot(shift, core):
    n = lax.axis_size("tp")
    me = lax.axis_index("tp")
    chip, mine = lax.div(me, CORES), lax.rem(me, CORES)
    chip = lax.rem(chip - shift + n // CORES, n // CORES)
    return chip * CORES + (mine if core == 0 else 1 - mine)


def source_row(shift):
    n = lax.axis_size("sp")
    return lax.rem(lax.axis_index("sp") - shift + n, n)


def params(limit=14):
    return pltpu.CompilerParams(vmem_limit_bytes=limit * 2**20)


def vmem(count):
    return [pl.BlockSpec(memory_space=pltpu.VMEM)] * count


def norm_kernel(shifts, width, gain_ref, *refs):
    blocks, out_ref = refs[:-1], refs[-1]
    rows = out_ref.shape[0]
    total = out_ref.shape[1]
    tile = 16
    slots = [feature_slot(e, c) for e in range(shifts) for c in range(CORES)]

    def body(i, carry):
        at = pl.ds(pl.multiple_of(i * tile, tile), tile)
        parts = [b[at, :].astype(F32) for b in blocks]
        square = sum(p * p for p in parts)
        scale = lax.rsqrt(jnp.sum(square, axis=1, keepdims=True) / total + 1e-06)
        for slot, part in zip(slots, parts):
            cols = pl.ds(pl.multiple_of(slot * width, LANES), width)
            out_ref[at, cols] = (part * scale * gain_ref[:, cols]).astype(BF16)
        return carry

    lax.fori_loop(0, rows // tile, body, 0, unroll=2)


def normalize(blocks, gain):
    shifts = len(blocks)
    flat = [b for pair in blocks for b in pair]
    rows, width = flat[0].shape
    total = width * len(flat)
    return pl.pallas_call(
        functools.partial(norm_kernel, shifts, width),
        out_shape=jax.ShapeDtypeStruct((rows, total), BF16),
        in_specs=vmem(1 + len(flat)),
        out_specs=vmem(1)[0],
        compiler_params=params(),
        cost_estimate=pl.CostEstimate(
            flops=rows * total * 400, bytes_accessed=4 * rows * total, transcendentals=0
        ),
        name="norm",
    )(gain, *flat)


def conv_strip(glu_ref, taps, out_ref, cols, offset):
    kernel = taps.shape[0]
    rows = out_ref.shape[0]
    spread = [jnp.broadcast_to(taps[k : k + 1, :], (8, LANES)) for k in range(kernel)]
    by_shift = [
        [((k + offset) // 8, k) for k in range(kernel) if (k + offset) % 8 == s] for s in range(8)
    ]
    reach = (kernel - 1 + offset) // 8 + 1
    row_id = lax.broadcasted_iota(jnp.int32, (8, LANES), 0)

    def partials(i):
        window = [
            glu_ref[pl.ds(pl.multiple_of((i + q) * 8, 8), 8), cols] for q in range(reach)
        ]
        out = []
        for s, members in enumerate(by_shift):
            acc = None
            for q, k in members:
                term = spread[k] * window[q]
                acc = term if acc is None else acc + term
            if acc is None:
                acc = jnp.zeros((8, LANES), F32)
            out.append(acc if s == 0 else pltpu.roll(acc, 8 - s, 0))
        return out

    def merge(now, later):
        acc = now[0]
        for s in range(1, 8):
            acc = acc + jnp.where(row_id < 8 - s, now[s], later[s])
        return acc

    def body(j, now):
        middle = partials(2 * j + 1)
        later = partials(2 * j + 2)
        pair = jnp.concatenate([merge(now, middle), merge(middle, later)], axis=0)
        out_ref[pl.ds(pl.multiple_of(j * 16, 16), 16), cols] = pair.astype(BF16)
        return later

    lax.fori_loop(0, rows // 16, body, partials(0))


def glu_conv_kernel(spans, pad, layer, start, x_ref, *refs):
    vectors = refs[:CORES]
    local = refs[CORES : 3 * CORES]
    weights = refs[3 * CORES : -2]
    out_ref, glu_ref = refs[-2:]
    depth, width = weights[0].shape
    kernel = vectors[0].shape[1] - 2
    offset = pad - (kernel - 1) // 2
    first = (lax.axis_index("grp") == 0) | (lax.axis_size("grp") != 2)
    at = [pl.ds(pl.multiple_of(source_row(d) * depth, LANES), depth) for d in range(spans)]
    cols = slice(start, start + width)
    for core in range(CORES):
        own = x_ref[:, at[0]]
        sums = []
        for side in range(2):
            acc = None
            for d in range(1, spans):
                w = weights[(core * 2 + side) * (spans - 1) + d - 1]
                term = jnp.dot(x_ref[:, at[d]], w[...], preferred_element_type=F32)
                acc = term if acc is None else acc + term
            sums.append(acc)
        value = jnp.dot(own, local[core][layer, :, cols], preferred_element_type=F32)
        gate = jnp.dot(own, local[CORES + core][layer, :, cols], preferred_element_type=F32)
        value = value + jnp.where(first, sums[0], sums[1])
        gate = gate + jnp.where(first, sums[1], sums[0])
        glu_ref[:, core * width : (core + 1) * width] = value * jax.nn.sigmoid(gate)
        for strip in range(width // LANES):
            at_strip = start + strip * LANES
            conv_strip(
                glu_ref,
                vectors[core][layer, :kernel, at_strip : at_strip + LANES],
                out_ref,
                slice(core * width + strip * LANES, core * width + (strip + 1) * LANES),
                offset,
            )


def glu_conv(x, layer, start, vectors, local, weights, pad):
    spans = len(weights[0][0]) + 1
    flat = [w for core in weights for side in core for w in side]
    rows = x.shape[0]
    width = flat[0].shape[1]
    flops = 2 * rows * x.shape[1] * width * CORES * 2
    return pl.pallas_call(
        functools.partial(glu_conv_kernel, spans, pad, layer, start),
        out_shape=jax.ShapeDtypeStruct((rows - 2 * pad, CORES * width), BF16),
        in_specs=vmem(1 + 3 * CORES + len(flat)),
        out_specs=vmem(1)[0],
        scratch_shapes=[pltpu.VMEM((rows, CORES * width), F32)],
        compiler_params=params(),
        cost_estimate=pl.CostEstimate(
            flops=flops, bytes_accessed=2 * rows * x.shape[1], transcendentals=0
        ),
        name="glu_conv",
    )(x, *vectors, *local, *flat)


def act_kernel(shifts, halves, *refs):
    lns = refs[:shifts]
    blocks = refs[shifts:-1]
    out_ref = refs[-1]
    rows, total = out_ref.shape
    width = blocks[0].shape[1] // CORES
    tile = 16

    def body(i, carry):
        at = pl.ds(pl.multiple_of(i * tile, tile), tile)
        parts = [b[at, :].astype(F32) for b in blocks]
        mean = jnp.sum(sum(parts), axis=1, keepdims=True) / total
        square = jnp.sum(sum(p * p for p in parts), axis=1, keepdims=True) / total
        scale = lax.rsqrt(square - mean * mean + 1e-05)
        for e in range(shifts):
            for h in range(halves):
                part = parts[e * halves + h]
                for core in range(CORES):
                    own = part[:, core * width : (core + 1) * width]
                    gain = lns[e][core : core + 1, h * width : (h + 1) * width]
                    bias = lns[e][CORES + core : CORES + core + 1, h * width : (h + 1) * width]
                    shaped = (own - mean) * scale * gain + bias
                    start = feature_slot(e, core) * (width * halves) + h * width
                    cols = pl.ds(pl.multiple_of(start, LANES), width)
                    out_ref[at, cols] = (shaped * jax.nn.sigmoid(shaped)).astype(BF16)
        return carry

    lax.fori_loop(0, rows // tile, body, 0, unroll=2)


def activation(lns, blocks):
    shifts, halves = len(blocks), len(blocks[0])
    flat = [b for pair in blocks for b in pair]
    rows = flat[0].shape[0]
    total = sum(b.shape[1] for b in flat)
    return pl.pallas_call(
        functools.partial(act_kernel, shifts, halves),
        out_shape=jax.ShapeDtypeStruct((rows, total), BF16),
        in_specs=vmem(len(lns) + len(flat)),
        out_specs=vmem(1)[0],
        compiler_params=params(),
        cost_estimate=pl.CostEstimate(
            flops=rows * total * 800, bytes_accessed=4 * rows * total, transcendentals=0
        ),
        name="act",
    )(*lns, *flat)


def out_sum(spans, pad, layer, act_ref, res_ref, local_ref, weights):
    sides = len(weights) // (spans - 1)
    rows = act_ref.shape[0]
    depth = weights[0].shape[0]
    whole = local_ref.shape[1]
    group = lax.axis_index("grp")
    at = pl.ds(pl.multiple_of(source_row(0) * whole, LANES), whole)
    acc = jnp.dot(act_ref[:, at], local_ref[layer], preferred_element_type=F32)
    for d in range(1, spans):
        for side in range(sides):
            start = source_row(d) * whole
            if sides > 1:
                start = start + (group if side == 0 else 1 - group) * depth
            at = pl.ds(pl.multiple_of(start, LANES), depth)
            w = weights[side * (spans - 1) + d - 1]
            acc = acc + jnp.dot(act_ref[:, at], w[...], preferred_element_type=F32)
    return acc + res_ref[pad : pad + rows, :].astype(F32)


def out_kernel(spans, pad, layer, mask, span_rows, act_ref, res_ref, local_ref, *refs):
    weights, out_ref = refs[:-1], refs[-1]
    rows = out_ref.shape[0]
    acc = out_sum(spans, pad, layer, act_ref, res_ref, local_ref, weights)
    if mask:
        block = lax.axis_index("sp") * CORES + lax.rem(lax.axis_index("tp"), CORES)
        row = lax.broadcasted_iota(jnp.int32, (rows, 1), 0) - mask + block * span_rows
        inside = (row >= 0) & (row < span_rows * CORES * lax.axis_size("sp"))
        acc = jnp.where(inside, acc, 0.0)
    out_ref[...] = acc.astype(BF16)


def final_kernel(spans, pad, layer, act_ref, res_ref, local_ref, arrived_ref, *refs):
    weights, out_ref = refs[:-1], refs[-1]
    rows = act_ref.shape[0]
    core = lax.rem(lax.axis_index("tp"), CORES)
    acc = out_sum(spans, pad, layer, act_ref, res_ref, local_ref, weights)
    mine = pl.ds(pl.multiple_of(core * rows, 16), rows)
    theirs = pl.ds(pl.multiple_of((1 - core) * rows, 16), rows)
    out_ref[mine, :] = acc.astype(BF16)
    out_ref[theirs, :] = arrived_ref[...]


def project_out(act, res, layer, local, weights, pad, mask, span_rows, arrived=None):
    spans = len(weights[0]) + 1
    flat = [w for side in weights for w in side]
    rows = act.shape[0]
    width = res.shape[1]
    if arrived is None:
        kernel = functools.partial(out_kernel, spans, pad, layer, mask, span_rows)
        extra = []
    else:
        kernel = functools.partial(final_kernel, spans, pad, layer)
        extra = [arrived]
    return pl.pallas_call(
        kernel,
        out_shape=jax.ShapeDtypeStruct((rows * (1 + len(extra)), width), BF16),
        in_specs=vmem(3 + len(extra) + len(flat)),
        out_specs=vmem(1)[0],
        compiler_params=params(),
        cost_estimate=pl.CostEstimate(
            flops=2 * rows * act.shape[1] * width,
            bytes_accessed=2 * rows * act.shape[1],
            transcendentals=0,
        ),
        name="out",
    )(act, res, local, *extra, *flat)


def pick_kernel(plan, *refs):
    hbm, out, sem = refs[:3], refs[3:-1], refs[-1]
    group = lax.axis_index("grp")

    def move(ref, layer, rows, cols, k):
        return pltpu.make_async_copy(ref.at[layer, rows, cols], out[k], sem.at[k])

    for k, (layer, cols, flip) in enumerate(plan):
        if cols is None:
            depth = out[k].shape[0]
            at = group if not flip else 1 - group
            rows = pl.ds(pl.multiple_of(at * depth, 16), depth)
            move(hbm[2], layer, rows, slice(None), k).start()
        else:
            for which in range(2):

                @pl.when(group == (which if not flip else 1 - which))
                def _():
                    move(hbm[which], layer, slice(None), cols, k).start()

    for k, (layer, cols, flip) in enumerate(plan):
        if cols is None:
            depth = out[k].shape[0]
            move(hbm[2], layer, pl.ds(0, depth), slice(None), k).wait()
        else:
            move(hbm[0], layer, slice(None), cols, k).wait()


def pick(plan, shapes, w_value, w_gate, w_out):
    return pl.pallas_call(
        functools.partial(pick_kernel, plan),
        out_shape=[jax.ShapeDtypeStruct(s, BF16) for s in shapes],
        in_specs=[pl.BlockSpec(memory_space=pltpu.HBM)] * 3,
        out_specs=vmem(len(shapes)),
        scratch_shapes=[pltpu.SemaphoreType.DMA((len(shapes),))],
        compiler_params=params(),
        cost_estimate=pl.CostEstimate(flops=10**6, bytes_accessed=10**6, transcendentals=0),
        name="pick",
    )(w_value, w_gate, w_out)


def edges_kernel(rows, edge, tokens_ref, before_ref, after_ref, own_ref, theirs_ref):
    core = lax.rem(lax.axis_index("tp"), CORES)
    for which in range(CORES):

        @pl.when(core == which)
        def _():
            low, high = (own_ref, theirs_ref) if which == 0 else (theirs_ref, own_ref)
            low[:edge, :] = before_ref[...]
            low[edge:, :] = tokens_ref[: rows + edge, :]
            high[: rows + edge, :] = tokens_ref[rows - edge :, :]
            high[rows + edge :, :] = after_ref[...]


def with_edges(tokens, before, after, rows, edge):
    shape = jax.ShapeDtypeStruct((rows + 2 * edge, tokens.shape[1]), BF16)
    return pl.pallas_call(
        functools.partial(edges_kernel, rows, edge),
        out_shape=[shape, shape],
        in_specs=vmem(3),
        out_specs=vmem(2),
        compiler_params=params(),
        cost_estimate=pl.CostEstimate(flops=10**6, bytes_accessed=10**6, transcendentals=0),
        name="edges",
    )(tokens, before, after)


def gather_rows(mine, other, direct, swap):
    n = lax.axis_size("sp")
    upward = n // 2
    own = [[None] * n for _ in range(2 if swap else 1)]
    sib = [[None] * n for _ in range(2 if swap else 1)]

    held = mine
    for d in range(1, upward + 1):
        held = ring(held, "sp", 1)
        own[0][d] = held
    held = mine
    for d in range(1, n - upward):
        held = ring(held, "sp", -1)
        own[0][n - d] = held
    if direct:
        held = other
        for d in range(1, n - upward):
            held = ring(held, "sp", -1)
            own[1][n - d] = held
    for d in range(1, n):
        sib[0][d] = sibling(own[0][d])
        if not swap:
            continue
        if own[1][d] is None:
            own[1][d] = ring(own[0][d], "grp", 1)
            sib[1][d] = sibling(own[1][d])
        else:
            sib[1][d] = sibling(own[1][d])
    return [[side[1:] for side in own], [side[1:] for side in sib]]


def shards(tokens, norm_gain, w_value, w_gate, taps, ln_gain, ln_shift, w_out):
    layers = w_value.shape[0]
    kernel = taps.shape[1]
    half = (kernel - 1) // 2
    pad = -(-half // 16) * 16
    count, _ = tokens.shape
    rows = count // CORES
    edge = pad * layers
    chips = lax.axis_size("tp") // CORES
    depth = w_value.shape[1]
    chan = w_value.shape[2]
    halves = 2 if chan % (2 * LANES) == 0 else 1
    wide = chan // halves
    paired = lax.axis_size("grp") == 2
    split_rows = paired and (depth // 2) % LANES == 0

    plan, shapes = [], []
    for layer in range(layers):
        for h in range(halves):
            cols = slice(h * wide, (h + 1) * wide)
            for flip in (False, True) if layer == 0 or not paired else (False,):
                plan.append((layer, cols, flip))
                shapes.append((depth, wide))
        if split_rows:
            plan.append((layer, None, False))
            shapes.append((depth // 2, chan))
    blocks = dict(
        zip([(p[0], p[1] and p[1].start, p[2]) for p in plan],
            pick(tuple(plan), shapes, w_value, w_gate, w_out))
    )

    gathered = []
    for layer in range(layers):
        pieces = []
        for h in range(halves):
            mine = blocks[layer, h * wide, False]
            if paired:
                other = blocks.get((layer, h * wide, True))
                pieces.append(gather_rows(mine, other, layer == 0, True))
            else:
                a = gather_rows(w_value[layer][:, h * wide : (h + 1) * wide], None, False, False)
                b = gather_rows(w_gate[layer][:, h * wide : (h + 1) * wide], None, False, False)
                pieces.append([[a[0][0], b[0][0]], [a[1][0], b[1][0]]])
        if split_rows:
            closing = gather_rows(blocks[layer, None, False], None, False, True)
        else:
            closing = gather_rows(w_out[layer], None, False, False)
        gathered.append((pieces, closing))

    sib_value = sibling(w_value)
    sib_gate = sibling(w_gate)
    sib_out = sibling(w_out)
    vectors = jnp.concatenate([taps, ln_gain[:, None], ln_shift[:, None]], axis=1)
    sib_vectors = sibling(vectors)
    lns_own = jnp.concatenate(
        [
            vectors[:, kernel : kernel + 1],
            sib_vectors[:, kernel : kernel + 1],
            vectors[:, kernel + 1 :],
            sib_vectors[:, kernel + 1 :],
        ],
        axis=1,
    )
    lns = [lns_own] + [chip_shift(lns_own, e) for e in range(1, chips)]

    before = line(tokens[count - edge :], "sp", 1)
    after = line(tokens[:edge], "sp", -1)
    own, theirs = with_edges(tokens, before, after, rows, edge)
    stream = [own, sibling(theirs)]

    for layer in range(layers):
        last = layer == layers - 1
        pieces, closing = gathered[layer]
        moved = [stream] + [[chip_shift(s, e) for s in stream] for e in range(1, chips)]
        normed = normalize(moved, norm_gain[layer][None, :])
        convs = []
        for h in range(halves):
            convs.append(
                glu_conv(
                    normed,
                    layer,
                    h * wide,
                    [vectors, sib_vectors],
                    [w_value, sib_value, w_gate, sib_gate],
                    pieces[h],
                    pad,
                )
            )
        moved = [convs] + [[chip_shift(c, e) for c in convs] for e in range(1, chips)]
        act = activation([v[layer] for v in lns], moved)
        args = [(stream[c], layer, (w_out, sib_out)[c], closing[c], pad) for c in range(CORES)]
        if last:
            other = project_out(act, *args[1], 0, rows)
            arrived = sibling(other)
            return project_out(act, *args[0], 0, rows, arrived)
        mask = pad * (layers - 1 - layer)
        stream = [project_out(act, *args[c], mask, rows) for c in range(CORES)]


def solution(mesh):
    return jax.shard_map(
        shards,
        mesh=mesh,
        in_specs=(
            P(("grp", "sp"), "tp"),
            P(),
            P(None, "sp", "tp"),
            P(None, "sp", "tp"),
            P(None, None, "tp"),
            P(None, "tp"),
            P(None, "tp"),
            P(None, "sp", "tp"),
        ),
        out_specs=P(("grp", "sp"), "tp"),
        check_vma=False,
    )
```
